32 devices in a mesh: grp: 2 (over x), sp: 8 (over z, y), tp: 2 (over core).
Axes of the slice: x: 2, y: 2, z: 4, core: 2. Of those that a mesh axis runs over, the one named last changes fastest.
Arguments:
- tokens: bfloat16 [8192, 2048], P(('grp', 'sp', 'tp')), parts along dimension 0, may hold values from -60 to 60
- query_weight: bfloat16 [2048, 1024], P(None, 'tp'), may hold values from -0.125 to 0.125
- key_weight: bfloat16 [2048, 1024], P(None, 'tp'), may hold values from -0.125 to 0.125
- value_weight: bfloat16 [2048, 1024], P(None, 'tp'), may hold values from -0.125 to 0.125
- output_weight: bfloat16 [1024, 2048], P(None, 'tp'), may hold values from -1.5 to 1.5
Outputs:
- attended: bfloat16 [8192, 2048], P(('grp', 'sp'), 'tp'), parts along dimension 0
The draws below stay inside these ranges and needn't reach their ends.
There are 2 independent parts, one for each index of `grp`. The reference program is written for one: setup_inputs(seed, part) draws one part's arguments, and reference() takes and returns one part's arrays. A program takes and returns all parts, laid end to end along the dimension named above; an argument that names none is the same for every part. Nothing has to cross between parts.
All inputs are finite; a program needn't handle non-finite values.
Results may differ from the reference program's by a relative error of at most 0.012.
The reference program's roundings to bfloat16 on the way (of `queries`, `keys`, `values`, `weights` and `mixed`) count: a program that leaves them out, or rounds other values in their place, can miss the bound.
Values may be sent and summed in bfloat16 or wider, within the bound.
A program may use at most 128 MiB of HBM per device.

```python
import jax
import jax.numpy as jnp
from jax import lax

D = 2048
HEADS = 8
HEAD = 128
REACH_STEPS = 128
MIDDLE_DILATION = 4
FAR_DILATION = 16
TOKENS = 4096


def draw_tokens(key, part):
    key_base = jax.random.fold_in(key, 11)
    base = jnp.clip(jax.random.normal(key_base, (TOKENS, D), jnp.float32), -6.0, 6.0)
    return base.astype(jnp.bfloat16)


def steps_of(rng, shape, cuts, smallest, largest):
    gain, own = 1.0, jax.random.fold_in(rng, 6)
    for position, blocks in cuts:
        draws = jnp.exp(jax.random.uniform(jax.random.fold_in(own, position), (blocks,), jnp.float32, smallest / len(cuts), largest / len(cuts)))
        gain = gain * jnp.repeat(draws, shape[position] // blocks).reshape([-1 if axis == position else 1 for axis in range(len(shape))])
    return gain


def gaussian(key, extent, deviation, reach, shards=(), kind=jnp.bfloat16):
    factor_of = steps_of(key, extent, shards, -0.22, 0.18) if shards else 1.0
    entries = jax.random.normal(key, extent, jnp.float32) * deviation * factor_of
    return jnp.minimum(jnp.maximum(entries, -reach), reach).astype(kind)


def setup_inputs(seed: int = 0, part: int = 0) -> dict:
    key_of = jax.random.split(jax.random.key(seed), 6)
    own_keys = jax.random.split(jax.random.fold_in(key_of[5], part), 6)
    tokens = draw_tokens(jax.random.fold_in(jax.random.fold_in(key_of[5], part), 71), part)
    query_weight = gaussian(key_of[1], (D, HEADS * HEAD), D ** -0.5, 0.125, ((1, 2),))
    key_weight = gaussian(key_of[2], (D, HEADS * HEAD), D ** -0.5, 0.125, ((1, 2),))
    value_weight = gaussian(key_of[3], (D, HEADS * HEAD), D ** -0.5, 0.125, ((1, 2),))
    output_weight = gaussian(key_of[4], (HEADS * HEAD, D), (REACH_STEPS // 8) ** -0.5, 1.5, ((1, 2),))
    return dict(tokens=tokens, query_weight=query_weight, key_weight=key_weight, value_weight=value_weight, output_weight=output_weight)


THETA_BASE = 500000.0


def rotate(values, positions):
    half = values.shape[-1] // 2
    inverse = THETA_BASE ** (-jnp.arange(half, dtype=jnp.float32) / half)
    angles = positions[:, None, None] * inverse
    cosine = jnp.cos(angles)
    sine = jnp.sin(angles)
    first = values[..., :half]
    second = values[..., half:]
    return jnp.concatenate([first * cosine - second * sine, second * cosine + first * sine], axis=-1)


def pattern(queries, keys, values, pattern_dilation):
    length = queries.shape[0]
    unit = pattern_dilation * REACH_STEPS
    padded = -(-length // unit) * unit
    blocks = padded // unit

    def regroup(array):
        array = jnp.pad(array, ((0, padded - length), (0, 0), (0, 0)))
        return array.reshape(blocks, REACH_STEPS, pattern_dilation, HEADS, HEAD).astype(jnp.float32)

    def with_prev(array):
        earlier = jnp.pad(array, ((1, 0), (0, 0), (0, 0), (0, 0), (0, 0)))[:-1]
        return jnp.concatenate([earlier, array], axis=1)

    query_sub = regroup(queries)
    key_sub = with_prev(regroup(keys))
    value_sub = with_prev(regroup(values))
    scores = jnp.einsum('nqrhd,nkrhd->nrhqk', query_sub, key_sub) * HEAD ** -0.5
    query_index = jnp.arange(REACH_STEPS)[:, None] + REACH_STEPS
    key_index = jnp.arange(2 * REACH_STEPS)[None, :]
    distance = query_index - key_index
    key_global = jnp.arange(blocks)[:, None, None] * REACH_STEPS + key_index[None] - REACH_STEPS
    allowed = ((distance >= 0) & (distance <= REACH_STEPS))[None] & (key_global >= 0)
    scores = jnp.where(allowed[:, None, None], scores, -jnp.inf)
    top = jnp.max(scores, axis=-1, keepdims=True)
    offset_keys = jnp.exp(scores - top)
    total = jnp.sum(offset_keys, axis=-1, keepdims=True)
    weights = lax.optimization_barrier((offset_keys / total).astype(jnp.bfloat16)).astype(jnp.float32)
    result = jnp.einsum('nrhqk,nkrhd->nqrhd', weights, value_sub).reshape(padded, HEADS, HEAD)[:length]
    lse = jnp.transpose((top + jnp.log(total))[..., 0], (0, 3, 1, 2)).reshape(padded, HEADS)[:length]
    return result, lse


def reference(tokens, query_weight, key_weight, value_weight, output_weight):
    length = tokens.shape[0]
    positions = jnp.arange(length).astype(jnp.float32)
    query_proj = jnp.dot(tokens, query_weight, preferred_element_type=jnp.float32).reshape(length, HEADS, HEAD)
    key_proj = jnp.dot(tokens, key_weight, preferred_element_type=jnp.float32).reshape(length, HEADS, HEAD)
    queries = rotate(query_proj, positions).astype(jnp.bfloat16)
    keys = rotate(key_proj, positions).astype(jnp.bfloat16)
    values = jnp.dot(tokens, value_weight, preferred_element_type=jnp.float32).astype(jnp.bfloat16)
    values = values.reshape(length, HEADS, HEAD)
    results = []
    lses = []
    for pattern_dilation in (1, MIDDLE_DILATION, FAR_DILATION):
        result, lse = pattern(queries, keys, values, pattern_dilation)
        results.append(result)
        lses.append(lse)
    mixing = jax.nn.softmax(jnp.stack(lses, axis=0), axis=0)
    mixed = jnp.sum(mixing[..., None] * jnp.stack(results, axis=0), axis=0)
    mixed = mixed.astype(jnp.bfloat16).reshape(length, HEADS * HEAD)
    return jnp.dot(mixed, output_weight, preferred_element_type=jnp.float32).astype(jnp.bfloat16)
```

```python
import functools

import jax
import jax.numpy as jnp
from jax import lax
from jax.experimental import pallas as pl
from jax.experimental.pallas import tpu as pltpu
from jax.sharding import PartitionSpec as P

HEAD = 128
REACH_STEPS = 128
MIDDLE_DILATION = 4
FAR_DILATION = 16
THETA_BASE = 500000.0
NEG = -1e30
MESH = pl.DeviceIdType.MESH
F32 = jnp.float32
BF16 = jnp.bfloat16

B, D, A, C, O = 0, 1, 2, 3, 4
SLOTS = 5
CLASSES = MIDDLE_DILATION
CLASS_ROWS = 128


def spot(i):
    return (i >> 6) * 256 + (i & 15) * 16 + ((i >> 4) & 3) * 4


def iota(shape, dim):
    return lax.broadcasted_iota(jnp.int32, shape, dim)


def rotated(x, cosine, sine):
    return x * cosine + pltpu.roll(x, HEAD // 2, 1) * sine


def softmax(scores, values):
    top = jnp.max(scores, axis=-1, keepdims=True)
    raised = jnp.exp(scores - top)
    total = jnp.sum(raised, axis=-1, keepdims=True)
    weights = (raised * (1.0 / total)).astype(BF16)
    result = jnp.dot(weights, values, preferred_element_type=F32)
    return result, top + jnp.log(total)


def transposed_dot(a, b):
    return lax.dot_general(a, b, (((1,), (1,)), ((), ())), preferred_element_type=F32)


def kernel(
    n_sp, heads,
    tok_hbm, wq_hbm, wk_hbm, wv_hbm, wo_hbm, cos_ref, sin_ref,
    out_ref,
    tok, wkv, wq, wo, xg, ctx, q, k1, v1, perm, unperm, b16, b4, b1, mixp, mixg,
    load_sem, x_sem, ctx_send, ctx_recv, mix_send, mix_recv,
):
    sp = lax.axis_index("sp")
    tp = lax.axis_index("tp")
    z = sp // 2
    odd = sp % 2
    even = odd == 0
    other = 1 - tp
    has_next = z + 1 < n_sp // 2

    tok_copy = pltpu.make_async_copy(tok_hbm, tok, load_sem.at[0])
    tok_copy.start()
    kv_copies = []
    for h in range(heads):
        cols = pl.ds(h * HEAD, HEAD)
        pair = (
            pltpu.make_async_copy(wk_hbm.at[:, cols], wkv.at[h, :, pl.ds(0, HEAD)], load_sem.at[1 + 2 * h]),
            pltpu.make_async_copy(wv_hbm.at[:, cols], wkv.at[h, :, pl.ds(HEAD, HEAD)], load_sem.at[2 + 2 * h]),
        )
        for copy in pair:
            copy.start()
        kv_copies.append(pair)
    q_copies = []
    for p in range(heads // 2):
        copy = pltpu.make_async_copy(
            wq_hbm.at[:, pl.ds(p * 2 * HEAD, 2 * HEAD)], wq.at[p], load_sem.at[1 + 2 * heads + p])
        copy.start()
        q_copies.append(copy)
    wo_copy = pltpu.make_async_copy(wo_hbm, wo, load_sem.at[1 + 2 * heads + heads // 2])
    wo_copy.start()

    barrier = pltpu.get_barrier_semaphore()
    y_partner = sp + 1 - 2 * odd

    def greet(ids):
        pl.semaphore_signal(barrier, inc=1, device_id=ids, device_id_type=MESH)

    greet({"tp": other})
    greet({"sp": y_partner})

    @pl.when(has_next)
    def _():
        greet({"sp": sp + 2})

    @pl.when(z > 0)
    def _():
        greet({"sp": sp - 2})

    row = iota((256, 256), 0)
    perm[...] = jnp.where(spot(row & 63) + (row >> 6) == iota((256, 256), 1), 1.0, 0.0).astype(BF16)

    pl.semaphore_wait(barrier, 2 + has_next.astype(jnp.int32) + (z > 0).astype(jnp.int32))

    tok_copy.wait()
    width = tok.shape[1]

    def reorder(i, _):
        cols = pl.ds(pl.multiple_of(i * 512, 512), 512)
        moved = jnp.dot(perm[...], tok[:, cols], preferred_element_type=F32).astype(BF16)
        xg[:, tp, :, cols] = moved.reshape(CLASSES, 64, 512)
        return 0

    lax.fori_loop(0, width // 512, reorder, 0)
    x_copy = pltpu.make_async_remote_copy(
        src_ref=xg.at[:, tp], dst_ref=xg.at[:, tp], send_sem=x_sem.at[0], recv_sem=x_sem.at[1],
        device_id={"tp": other}, device_id_type=MESH)
    x_copy.start()

    qi, kj = iota((128, 640), 0), iota((128, 640), 1)
    dist = 4 - (kj >> 7)
    diff = spot(qi) - spot(kj & 127) + 512 * dist
    here = dist <= sp
    far = here & ((diff & 15) == 0) & (diff >= 0) & (diff <= FAR_DILATION * REACH_STEPS)
    b16[...] = jnp.where(far, 0.0, NEG)
    mid = here & (diff >= 0) & (diff <= MIDDLE_DILATION * REACH_STEPS)
    b4[...] = jnp.where(mid, 0.0, NEG)[:, 384:]
    key_spot = jnp.where(kj < 128, kj - 128, spot(kj & 127) + ((kj >> 7) - 1))
    for c in range(CLASSES):
        near = spot(qi) + c - key_spot
        ok = (near >= 0) & (near <= REACH_STEPS) & ((kj >= 128) | (sp > 0))
        b1[c] = jnp.where(ok, 0.0, NEG)
    col = iota((512, 512), 1)
    unperm[...] = jnp.where(spot(col & 127) + (col >> 7) == iota((512, 512), 0), 1.0, 0.0).astype(BF16)

    for slot in (B, D, A, C):
        @pl.when(sp < 4 - slot)
        def _():
            def clear(h, _):
                ctx[h, :, :, slot] = jnp.zeros((2, CLASSES, 128, HEAD), BF16)
                return 0
            lax.fori_loop(0, heads, clear, 0)

    def send(h, src, dst, ids):
        return pltpu.make_async_remote_copy(
            src_ref=ctx.at[h, :, :, src], dst_ref=ctx.at[h, :, :, dst],
            send_sem=ctx_send.at[dst, h], recv_sem=ctx_recv.at[dst, h],
            device_id=ids, device_id_type=MESH)

    down = {"sp": sp + 2}
    side = {"sp": y_partner}

    def sends_of(h, src):
        if src == O:
            return [(has_next, send(h, O, A, down)), (even, send(h, O, C, side))]
        if src == A:
            return [(has_next & (z > 0), send(h, A, B, down)),
                    (even & (z > 0), send(h, A, D, side)),
                    ((odd == 1) & (z > 0), send(h, A, C, side))]
        return [((odd == 1) & (z > 1), send(h, B, D, side))]

    def start_all(h, src):
        for condition, copy in sends_of(h, src):
            @pl.when(condition)
            def _():
                copy.start()

    def receive(h, slot):
        @pl.when(sp >= 4 - slot)
        def _():
            send(h, slot, slot, side).wait_recv()

    x_copy.wait_recv()

    def tokens():
        return xg[...].reshape(512, width)

    def project_kv(h, _):
        kv = jnp.dot(tokens(), wkv[h], preferred_element_type=F32)
        k = rotated(kv[:, :HEAD], cos_ref[...], sin_ref[...]).astype(BF16)
        ctx[h, 0, :, O] = k.reshape(CLASSES, 128, HEAD)
        ctx[h, 1, :, O] = kv[:, HEAD:].astype(BF16).reshape(CLASSES, 128, HEAD)
        start_all(h, O)
        return 0

    for pair in kv_copies:
        for copy in pair:
            copy.wait()
    lax.fori_loop(0, heads, project_kv, 0)

    for copy in q_copies:
        copy.wait()

    def project_q(p, _):
        qq = jnp.dot(tokens(), wq[p], preferred_element_type=F32)
        for s in range(2):
            r = rotated(qq[:, s * HEAD:(s + 1) * HEAD], cos_ref[...], sin_ref[...])
            q[2 * p + s] = r.astype(BF16).reshape(CLASSES, 128, HEAD)
        return 0

    lax.fori_loop(0, heads // 2, project_q, 0)

    def relay(h, _):
        receive(h, A)
        start_all(h, A)
        return 0

    lax.fori_loop(0, heads, relay, 0)

    def mix_copy(h):
        cols = pl.ds(pl.multiple_of(h * HEAD, HEAD), HEAD)
        return pltpu.make_async_remote_copy(
            src_ref=mixg.at[tp, :, cols], dst_ref=mixg.at[tp, :, cols],
            send_sem=mix_send.at[h], recv_sem=mix_recv.at[h],
            device_id={"tp": other}, device_id_type=MESH)

    def attend(h, _):
        receive(h, B)
        start_all(h, B)
        receive(h, C)
        receive(h, D)
        tail = unperm[384:512, :]
        for kv, near in ((0, k1), (1, v1)):
            last = ctx[h, kv, :, C].reshape(512, HEAD)
            near[0:128] = jnp.dot(tail, last, preferred_element_type=F32).astype(BF16)
            near[128:640] = ctx[h, kv, :, O].reshape(512, HEAD)

        def of_class(c, _):
            qc = q[h, c]
            keys = ctx[h, 0, c].reshape(SLOTS * 128, HEAD)
            vals = ctx[h, 1, c].reshape(SLOTS * 128, HEAD)
            scores = transposed_dot(qc, keys) * HEAD ** (-0.5)
            r16, l16 = softmax(scores + b16[...], vals)
            r4, l4 = softmax(scores[:, 384:] + b4[...], vals[384:])
            r1, l1 = softmax(transposed_dot(qc, k1[...]) * HEAD ** (-0.5) + b1[c], v1[...])
            most = jnp.maximum(jnp.maximum(l16, l4), l1)
            e16, e4, e1 = jnp.exp(l16 - most), jnp.exp(l4 - most), jnp.exp(l1 - most)
            share = 1.0 / (e16 + e4 + e1)
            mixed = r1 * (e1 * share) + r4 * (e4 * share) + r16 * (e16 * share)
            mixp[pl.ds(pl.multiple_of(c * 128, 128), 128), :] = mixed.astype(BF16)
            return 0

        lax.fori_loop(0, CLASSES, of_class, 0)
        natural = jnp.dot(unperm[...], mixp[...], preferred_element_type=F32).astype(BF16)
        cols = pl.ds(pl.multiple_of(h * HEAD, HEAD), HEAD)
        mixg[tp, :, cols] = natural
        mix_copy(h).start()
        return 0

    lax.fori_loop(0, heads, attend, 0)

    wo_copy.wait()

    def gathered(h, _):
        mix_copy(h).wait_recv()
        return 0

    lax.fori_loop(0, heads, gathered, 0)
    half = mixg.shape[2]

    def project_out(i, _):
        cols = pl.ds(pl.multiple_of(i * 256, 256), 256)
        total = jnp.dot(mixg[0], wo[:half, cols], preferred_element_type=F32)
        total = total + jnp.dot(mixg[1], wo[half:, cols], preferred_element_type=F32)
        out_ref[:, cols] = total.astype(BF16)
        return 0

    lax.fori_loop(0, out_ref.shape[1] // 256, project_out, 0)

    x_copy.wait_send()

    def left(h, _):
        for src in (O, A, B):
            for condition, copy in sends_of(h, src):
                @pl.when(condition)
                def _():
                    copy.wait_send()
        mix_copy(h).wait_send()
        return 0

    lax.fori_loop(0, heads, left, 0)


def body(tokens, query_weight, key_weight, value_weight, output_weight):
    n_sp = lax.axis_size("sp")
    half_rows, width = tokens.shape
    rows = half_rows * lax.axis_size("tp")
    heads = query_weight.shape[1] // HEAD
    assert rows * 4 == FAR_DILATION * REACH_STEPS and rows == 512
    assert n_sp % 2 == 0 and lax.axis_size("tp") == 2 and heads % 2 == 0

    index = jnp.arange(rows, dtype=jnp.int32)
    positions = lax.axis_index("sp") * rows + spot(index & 127) + (index >> 7)
    half = HEAD // 2
    inverse = THETA_BASE ** (-jnp.arange(half, dtype=F32) / half)
    angles = positions.astype(F32)[:, None] * inverse
    cosine, sine = jnp.cos(angles), jnp.sin(angles)
    cos_table = jnp.concatenate([cosine, cosine], axis=1)
    sin_table = jnp.concatenate([-sine, sine], axis=1)

    anywhere = pl.BlockSpec(memory_space=pl.ANY)
    vmem = pl.BlockSpec(memory_space=pltpu.VMEM)
    out_cols = output_weight.shape[1]
    return pl.pallas_call(
        functools.partial(kernel, n_sp, heads),
        out_shape=jax.ShapeDtypeStruct((rows, out_cols), BF16),
        in_specs=[anywhere] * 5 + [vmem] * 2,
        out_specs=vmem,
        scratch_shapes=[
            pltpu.VMEM((half_rows, width), BF16),
            pltpu.VMEM((heads, width, 2 * HEAD), BF16),
            pltpu.VMEM((heads // 2, width, 2 * HEAD), BF16),
            pltpu.VMEM(output_weight.shape, BF16),
            pltpu.VMEM((CLASSES, 2, 64, width), BF16),
            pltpu.VMEM((heads, 2, CLASSES, SLOTS, 128, HEAD), BF16),
            pltpu.VMEM((heads, CLASSES, 128, HEAD), BF16),
            pltpu.VMEM((640, HEAD), BF16),
            pltpu.VMEM((640, HEAD), BF16),
            pltpu.VMEM((256, 256), BF16),
            pltpu.VMEM((512, 512), BF16),
            pltpu.VMEM((128, 640), F32),
            pltpu.VMEM((128, 256), F32),
            pltpu.VMEM((CLASSES, 128, 640), F32),
            pltpu.VMEM((512, HEAD), BF16),
            pltpu.VMEM((2, rows, heads * HEAD), BF16),
            pltpu.SemaphoreType.DMA((2 + 2 * heads + heads // 2,)),
            pltpu.SemaphoreType.DMA((2,)),
            pltpu.SemaphoreType.DMA((4, heads)),
            pltpu.SemaphoreType.DMA((4, heads)),
            pltpu.SemaphoreType.DMA((heads,)),
            pltpu.SemaphoreType.DMA((heads,)),
        ],
        compiler_params=pltpu.CompilerParams(
            collective_id=0, has_side_effects=True, vmem_limit_bytes=48 * 1024 * 1024
        ),
    )(tokens, query_weight, key_weight, value_weight, output_weight, cos_table, sin_table)


def solution(mesh):
    in_specs = (
        P(("grp", "sp", "tp"), None),
        P(None, "tp"),
        P(None, "tp"),
        P(None, "tp"),
        P(None, "tp"),
    )
    out_specs = P(("grp", "sp"), "tp")
    return jax.shard_map(body, mesh=mesh, in_specs=in_specs, out_specs=out_specs, check_vma=False)
```

```python
import functools

import jax
import jax.numpy as jnp
import numpy as np
from jax import lax
from jax.experimental import pallas as pl
from jax.experimental.pallas import tpu as pltpu
from jax.sharding import PartitionSpec as P

HEAD = 128
REACH_STEPS = 128
MIDDLE_DILATION = 4
FAR_DILATION = 16
THETA_BASE = 500000.0
NEG = -1e30
MESH = pl.DeviceIdType.MESH
F32 = jnp.float32
BF16 = jnp.bfloat16

A, C, O = 0, 1, 2
SLOTS = 3
CLASSES = MIDDLE_DILATION
CLASS_ROWS = 128


def spot(i):
    return (i >> 6) * 256 + (i & 15) * 16 + ((i >> 4) & 3) * 4


def iota(shape, dim):
    return lax.broadcasted_iota(jnp.int32, shape, dim)


def rotated(x, cosine, sine):
    return x * cosine + pltpu.roll(x, HEAD // 2, 1) * sine


def softmax(scores, values):
    top = jnp.max(scores, axis=-1, keepdims=True)
    raised = jnp.exp(scores - top)
    total = jnp.sum(raised, axis=-1, keepdims=True)
    weights = (raised * (1.0 / total)).astype(BF16)
    result = jnp.dot(weights, values, preferred_element_type=F32)
    return result, top + jnp.log(total)


def transposed_dot(a, b):
    return lax.dot_general(a, b, (((1,), (1,)), ((), ())), preferred_element_type=F32)


def kernel(
    n_sp, heads,
    tok_hbm, wq_hbm, wk_hbm, wv_hbm, wo_hbm, inv_hbm,
    out_ref,
    tok, wkv, wq, wo, inv, cos_ref, sin_ref, xg, ctx, q, visitor, k1, v1, perm, unperm,
    b16, b4, b1, near_out, near_lse, part, part_lse, far_out, far_lse, mixp, mixg,
    load_sem, x_sem, ctx_send, ctx_recv, q_sem, part_sem, lse_sem, mix_send, mix_recv,
):
    sp = lax.axis_index("sp")
    tp = lax.axis_index("tp")
    z = sp // 2
    odd = sp % 2
    even = odd == 0
    other = 1 - tp
    has_next = z + 1 < n_sp // 2

    tok_copy = pltpu.make_async_copy(tok_hbm, tok, load_sem.at[0])
    tok_copy.start()
    inv_copy = pltpu.make_async_copy(inv_hbm, inv, load_sem.at[2 + 2 * heads + heads // 2])
    inv_copy.start()
    kv_copies = []
    for h in range(heads):
        cols = pl.ds(h * HEAD, HEAD)
        pair = (
            pltpu.make_async_copy(wk_hbm.at[:, cols], wkv.at[h, :, pl.ds(0, HEAD)], load_sem.at[1 + 2 * h]),
            pltpu.make_async_copy(wv_hbm.at[:, cols], wkv.at[h, :, pl.ds(HEAD, HEAD)], load_sem.at[2 + 2 * h]),
        )
        for copy in pair:
            copy.start()
        kv_copies.append(pair)
    q_copies = []
    for p in range(heads // 2):
        copy = pltpu.make_async_copy(
            wq_hbm.at[:, pl.ds(p * 2 * HEAD, 2 * HEAD)], wq.at[p], load_sem.at[1 + 2 * heads + p])
        copy.start()
        q_copies.append(copy)
    wo_copy = pltpu.make_async_copy(wo_hbm, wo, load_sem.at[1 + 2 * heads + heads // 2])
    wo_copy.start()

    barrier = pltpu.get_barrier_semaphore()
    y_partner = sp + 1 - 2 * odd

    def greet(ids):
        pl.semaphore_signal(barrier, inc=1, device_id=ids, device_id_type=MESH)

    greet({"tp": other})
    greet({"sp": y_partner})

    @pl.when(has_next)
    def _():
        greet({"sp": sp + 2})

    @pl.when(z > 0)
    def _():
        greet({"sp": sp - 2})

    row = iota((256, 256), 0)
    perm[...] = jnp.where(spot(row & 63) + (row >> 6) == iota((256, 256), 1), 1.0, 0.0).astype(BF16)

    pl.semaphore_wait(barrier, 2 + has_next.astype(jnp.int32) + (z > 0).astype(jnp.int32))

    tok_copy.wait()
    width = tok.shape[1]

    def reorder(i, _):
        cols = pl.ds(pl.multiple_of(i * 512, 512), 512)
        moved = jnp.dot(perm[...], tok[:, cols], preferred_element_type=F32).astype(BF16)
        xg[:, tp, :, cols] = moved.reshape(CLASSES, 64, 512)
        return 0

    lax.fori_loop(0, width // 512, reorder, 0)
    x_copy = pltpu.make_async_remote_copy(
        src_ref=xg.at[:, tp], dst_ref=xg.at[:, tp], send_sem=x_sem.at[0], recv_sem=x_sem.at[1],
        device_id={"tp": other}, device_id_type=MESH)
    x_copy.start()

    inv_copy.wait()
    lane = iota((128, HEAD), 1)

    def table(c, _):
        positions = sp * 512 + spot(iota((128, HEAD), 0)) + c
        angles = positions.astype(F32) * inv[...]
        rows = pl.ds(pl.multiple_of(c * 128, 128), 128)
        cos_ref[rows, :] = jnp.cos(angles)
        sine = jnp.sin(angles)
        sin_ref[rows, :] = jnp.where(lane < HEAD // 2, -sine, sine)
        return 0

    lax.fori_loop(0, CLASSES, table, 0)

    qi, kj = iota((128, 640), 0), iota((128, 640), 1)
    dist = 4 - (kj >> 7)
    diff = spot(qi) - spot(kj & 127) + 512 * dist
    here = (dist <= sp) | ((dist >= 3) & (dist <= sp + 2))
    far = here & ((diff & 15) == 0) & (diff >= 0) & (diff <= FAR_DILATION * REACH_STEPS)
    b16[...] = jnp.where(far, 0.0, NEG)
    mid = here & (diff >= 0) & (diff <= MIDDLE_DILATION * REACH_STEPS)
    b4[...] = jnp.where(mid, 0.0, NEG)[:, 384:]
    key_spot = jnp.where(kj < 128, kj - 128, spot(kj & 127) + ((kj >> 7) - 1))
    for c in range(CLASSES):
        near = spot(qi) + c - key_spot
        ok = (near >= 0) & (near <= REACH_STEPS) & ((kj >= 128) | (sp > 0))
        b1[c] = jnp.where(ok, 0.0, NEG)
    col = iota((512, 512), 1)
    unperm[...] = jnp.where(spot(col & 127) + (col >> 7) == iota((512, 512), 0), 1.0, 0.0).astype(BF16)

    for slot in (A, C):
        @pl.when(sp < 2 - slot)
        def _():
            def clear(h, _):
                ctx[h, :, :, slot] = jnp.zeros((2, CLASSES, 128, HEAD), BF16)
                return 0
            lax.fori_loop(0, heads, clear, 0)

    part_lse[...] = jnp.zeros(part_lse.shape, F32)

    @pl.when(z == 0)
    def _():
        far_out[...] = jnp.zeros(far_out.shape, BF16)
        far_lse[...] = jnp.full(far_lse.shape, NEG, F32)

    def remote(src, dst, send_sem, recv_sem, ids):
        return pltpu.make_async_remote_copy(
            src_ref=src, dst_ref=dst, send_sem=send_sem, recv_sem=recv_sem,
            device_id=ids, device_id_type=MESH)

    down = {"sp": sp + 2}
    up = {"sp": sp - 2}
    side = {"sp": y_partner}

    def send(h, src, dst, ids):
        return remote(ctx.at[h, :, :, src], ctx.at[h, :, :, dst],
                      ctx_send.at[dst, h], ctx_recv.at[dst, h], ids)

    def send_own(h):
        return ((has_next, send(h, O, A, down)), (even, send(h, O, C, side)))

    def send_relay(h):
        return (((odd == 1) & (z > 0), send(h, A, C, side)),)

    def send_query(h):
        return ((z > 0, remote(q.at[h], visitor.at[h], q_sem.at[0, h], q_sem.at[1, h], up)),)

    def send_part(h):
        return ((has_next, remote(part.at[h], far_out.at[h], part_sem.at[0, h], part_sem.at[1, h], down)),
                (has_next, remote(part_lse.at[h], far_lse.at[h], lse_sem.at[0, h], lse_sem.at[1, h], down)))

    def start_all(sends):
        for condition, copy in sends:
            @pl.when(condition)
            def _():
                copy.start()

    def receive(h, slot):
        @pl.when(sp >= 2 - slot)
        def _():
            send(h, slot, slot, side).wait_recv()

    x_copy.wait_recv()

    def tokens():
        return xg[...].reshape(512, width)

    def project_kv(h, _):
        kv = jnp.dot(tokens(), wkv[h], preferred_element_type=F32)
        k = rotated(kv[:, :HEAD], cos_ref[...], sin_ref[...]).astype(BF16)
        ctx[h, 0, :, O] = k.reshape(CLASSES, 128, HEAD)
        ctx[h, 1, :, O] = kv[:, HEAD:].astype(BF16).reshape(CLASSES, 128, HEAD)
        start_all(send_own(h))
        return 0

    for pair in kv_copies:
        for copy in pair:
            copy.wait()
    lax.fori_loop(0, heads, project_kv, 0)

    for copy in q_copies:
        copy.wait()

    def project_q(p, _):
        qq = jnp.dot(tokens(), wq[p], preferred_element_type=F32)
        for s in range(2):
            r = rotated(qq[:, s * HEAD:(s + 1) * HEAD], cos_ref[...], sin_ref[...])
            q[2 * p + s] = r.astype(BF16).reshape(CLASSES, 128, HEAD)
            start_all(send_query(2 * p + s))
        return 0

    lax.fori_loop(0, heads // 2, project_q, 0)

    def mix_copy(h):
        cols = pl.ds(pl.multiple_of(h * HEAD, HEAD), HEAD)
        return pltpu.make_async_remote_copy(
            src_ref=mixg.at[tp, :, cols], dst_ref=mixg.at[tp, :, cols],
            send_sem=mix_send.at[h], recv_sem=mix_recv.at[h],
            device_id={"tp": other}, device_id_type=MESH)

    eye = iota((128, 128), 0) == iota((128, 128), 1)

    def visit(h):
        @pl.when(has_next)
        def _():
            remote(q.at[h], visitor.at[h], q_sem.at[0, h], q_sem.at[1, h], side).wait_recv()

            def of_class(c, _):
                keys = ctx[h, 0, c, A:O].reshape(2 * 128, HEAD)
                vals = ctx[h, 1, c, A:O].reshape(2 * 128, HEAD)
                scores = transposed_dot(visitor[h, c], keys) * HEAD ** (-0.5)
                result, lse = softmax(scores + b16[:, :256], vals)
                part[h, c] = result.astype(BF16)
                part_lse[h, pl.ds(c, 1), :] = jnp.sum(jnp.where(eye, lse, 0.0), axis=0, keepdims=True)
                return 0

            lax.fori_loop(0, CLASSES, of_class, 0)

        start_all(send_part(h))

    def attend(h):
        tail = unperm[384:512, :]
        for kv, near in ((0, k1), (1, v1)):
            last = ctx[h, kv, :, C].reshape(512, HEAD)
            near[0:128] = jnp.dot(tail, last, preferred_element_type=F32).astype(BF16)
            near[128:640] = ctx[h, kv, :, O].reshape(512, HEAD)

        def of_class(c, _):
            qc = q[h, c]
            keys = ctx[h, 0, c].reshape(SLOTS * 128, HEAD)
            vals = ctx[h, 1, c].reshape(SLOTS * 128, HEAD)
            scores = transposed_dot(qc, keys) * HEAD ** (-0.5)
            r16, l16 = softmax(scores + b16[:, 256:], vals)
            r4, l4 = softmax(scores[:, 128:] + b4[...], vals[128:])
            r1, l1 = softmax(transposed_dot(qc, k1[...]) * HEAD ** (-0.5) + b1[c], v1[...])
            most = jnp.maximum(jnp.maximum(l16, l4), l1)
            e16, e4, e1 = jnp.exp(l16 - most), jnp.exp(l4 - most), jnp.exp(l1 - most)
            total = e16 + e4 + e1
            share = 1.0 / total
            near_out[h, c] = r1 * (e1 * share) + r4 * (e4 * share) + r16 * (e16 * share)
            near_lse[h, c] = jnp.broadcast_to(most + jnp.log(total), (128, HEAD))
            return 0

        lax.fori_loop(0, CLASSES, of_class, 0)

    def step(h, _):
        @pl.when(h < heads)
        def _():
            receive(h, A)
            start_all(send_relay(h))

        @pl.when(h > 0)
        def _():
            receive(h - 1, C)
            visit(h - 1)
            attend(h - 1)
        return 0

    lax.fori_loop(0, heads + 1, step, 0)

    def combine(h, _):
        @pl.when(z > 0)
        def _():
            remote(part.at[h], far_out.at[h], part_sem.at[0, h], part_sem.at[1, h], side).wait_recv()
            remote(part_lse.at[h], far_lse.at[h], lse_sem.at[0, h], lse_sem.at[1, h], side).wait_recv()

        for c in range(CLASSES):
            row = far_lse[h, c:c + 1, :]
            lf = jnp.sum(jnp.where(eye, row, 0.0), axis=1, keepdims=True)
            ln = near_lse[h, c]
            most = jnp.maximum(ln, lf)
            en, ef = jnp.exp(ln - most), jnp.exp(lf - most)
            mixed = (near_out[h, c] * en + far_out[h, c].astype(F32) * ef) / (en + ef)
            mixp[c * 128:(c + 1) * 128, :] = mixed.astype(BF16)
        natural = jnp.dot(unperm[...], mixp[...], preferred_element_type=F32).astype(BF16)
        cols = pl.ds(pl.multiple_of(h * HEAD, HEAD), HEAD)
        mixg[tp, :, cols] = natural
        mix_copy(h).start()
        return 0

    lax.fori_loop(0, heads, combine, 0)

    wo_copy.wait()

    def gathered(h, _):
        mix_copy(h).wait_recv()
        return 0

    lax.fori_loop(0, heads, gathered, 0)
    half = mixg.shape[2]

    def project_out(i, _):
        cols = pl.ds(pl.multiple_of(i * 256, 256), 256)
        total = jnp.dot(mixg[0], wo[:half, cols], preferred_element_type=F32)
        total = total + jnp.dot(mixg[1], wo[half:, cols], preferred_element_type=F32)
        out_ref[:, cols] = total.astype(BF16)
        return 0

    lax.fori_loop(0, out_ref.shape[1] // 256, project_out, 0)

    x_copy.wait_send()

    def left(h, _):
        for sends in (send_own(h), send_relay(h), send_query(h), send_part(h)):
            for condition, copy in sends:
                @pl.when(condition)
                def _():
                    copy.wait_send()
        mix_copy(h).wait_send()
        return 0

    lax.fori_loop(0, heads, left, 0)


def body(tokens, query_weight, key_weight, value_weight, output_weight):
    n_sp = lax.axis_size("sp")
    half_rows, width = tokens.shape
    rows = half_rows * lax.axis_size("tp")
    heads = query_weight.shape[1] // HEAD
    assert rows * 4 == FAR_DILATION * REACH_STEPS and rows == 512
    assert n_sp % 2 == 0 and lax.axis_size("tp") == 2 and heads % 2 == 0

    half = HEAD // 2
    inverse = THETA_BASE ** (-np.arange(half, dtype=np.float64) / half)
    inverse = np.concatenate([inverse, inverse]).astype(np.float32)[None, :]

    anywhere = pl.BlockSpec(memory_space=pl.ANY)
    vmem = pl.BlockSpec(memory_space=pltpu.VMEM)
    out_cols = output_weight.shape[1]
    return pl.pallas_call(
        functools.partial(kernel, n_sp, heads),
        out_shape=jax.ShapeDtypeStruct((rows, out_cols), BF16),
        in_specs=[anywhere] * 6,
        out_specs=vmem,
        scratch_shapes=[
            pltpu.VMEM((half_rows, width), BF16),
            pltpu.VMEM((heads, width, 2 * HEAD), BF16),
            pltpu.VMEM((heads // 2, width, 2 * HEAD), BF16),
            pltpu.VMEM(output_weight.shape, BF16),
            pltpu.VMEM((1, HEAD), F32),
            pltpu.VMEM((rows, HEAD), F32),
            pltpu.VMEM((rows, HEAD), F32),
            pltpu.VMEM((CLASSES, 2, 64, width), BF16),
            pltpu.VMEM((heads, 2, CLASSES, SLOTS, 128, HEAD), BF16),
            pltpu.VMEM((heads, CLASSES, 128, HEAD), BF16),
            pltpu.VMEM((heads, CLASSES, 128, HEAD), BF16),
            pltpu.VMEM((640, HEAD), BF16),
            pltpu.VMEM((640, HEAD), BF16),
            pltpu.VMEM((256, 256), BF16),
            pltpu.VMEM((512, 512), BF16),
            pltpu.VMEM((128, 640), F32),
            pltpu.VMEM((128, 256), F32),
            pltpu.VMEM((CLASSES, 128, 640), F32),
            pltpu.VMEM((heads, CLASSES, 128, HEAD), F32),
            pltpu.VMEM((heads, CLASSES, 128, HEAD), F32),
            pltpu.VMEM((heads, CLASSES, 128, HEAD), BF16),
            pltpu.VMEM((heads, 8, 128), F32),
            pltpu.VMEM((heads, CLASSES, 128, HEAD), BF16),
            pltpu.VMEM((heads, 8, 128), F32),
            pltpu.VMEM((512, HEAD), BF16),
            pltpu.VMEM((2, rows, heads * HEAD), BF16),
            pltpu.SemaphoreType.DMA((3 + 2 * heads + heads // 2,)),
            pltpu.SemaphoreType.DMA((2,)),
            pltpu.SemaphoreType.DMA((2, heads)),
            pltpu.SemaphoreType.DMA((2, heads)),
            pltpu.SemaphoreType.DMA((2, heads)),
            pltpu.SemaphoreType.DMA((2, heads)),
            pltpu.SemaphoreType.DMA((2, heads)),
            pltpu.SemaphoreType.DMA((heads,)),
            pltpu.SemaphoreType.DMA((heads,)),
        ],
        compiler_params=pltpu.CompilerParams(
            collective_id=0, has_side_effects=True, vmem_limit_bytes=48 * 1024 * 1024
        ),
    )(tokens, query_weight, key_weight, value_weight, output_weight, jnp.asarray(inverse))


def solution(mesh):
    in_specs = (
        P(("grp", "sp", "tp"), None),
        P(None, "tp"),
        P(None, "tp"),
        P(None, "tp"),
        P(None, "tp"),
    )
    out_specs = P(("grp", "sp"), "tp")
    return jax.shard_map(body, mesh=mesh, in_specs=in_specs, out_specs=out_specs, check_vma=False)
```

```python
import functools

import jax
import jax.numpy as jnp
import numpy as np
from jax import lax
from jax.experimental import pallas as pl
from jax.experimental.pallas import tpu as pltpu
from jax.sharding import PartitionSpec as P

HEAD = 128
REACH_STEPS = 128
MIDDLE_DILATION = 4
FAR_DILATION = 16
THETA_BASE = 500000.0
NEG = -1e30
MESH = pl.DeviceIdType.MESH
F32 = jnp.float32
BF16 = jnp.bfloat16

A, C, O = 0, 1, 2
SLOTS = 3
CLASSES = MIDDLE_DILATION
CLASS_ROWS = 128


def spot(i):
    return (i >> 6) * 256 + (i & 15) * 16 + ((i >> 4) & 3) * 4


def iota(shape, dim):
    return lax.broadcasted_iota(jnp.int32, shape, dim)


def rotated(x, cosine, sine):
    return x * cosine + pltpu.roll(x, HEAD // 2, 1) * sine


def softmax(scores, values):
    top = jnp.max(scores, axis=-1, keepdims=True)
    raised = jnp.exp(scores - top)
    total = jnp.sum(raised, axis=-1, keepdims=True)
    weights = (raised * (1.0 / total)).astype(BF16)
    result = jnp.dot(weights, values, preferred_element_type=F32)
    return result, top + jnp.log(total)


def transposed_dot(a, b):
    return lax.dot_general(a, b, (((1,), (1,)), ((), ())), preferred_element_type=F32)


def kernel(
    n_sp, heads,
    tok_hbm, wq_hbm, wk_hbm, wv_hbm, wo_hbm, inv_hbm,
    out_ref,
    tok, wkv, wq, wo, inv, cos_ref, sin_ref, xg, ctx, q, visitor, k1, v1, perm, unperm,
    b16, b4, b1, near_out, near_lse, part, part_lse, far_out, far_lse, mixp, mixg, out_sum,
    load_sem, x_sem, ctx_send, ctx_recv, q_sem, part_sem, lse_sem, mix_send, mix_recv,
):
    sp = lax.axis_index("sp")
    tp = lax.axis_index("tp")
    z = sp // 2
    odd = sp % 2
    even = odd == 0
    other = 1 - tp
    has_next = z + 1 < n_sp // 2

    tok_copy = pltpu.make_async_copy(tok_hbm, tok, load_sem.at[0])
    tok_copy.start()
    inv_copy = pltpu.make_async_copy(inv_hbm, inv, load_sem.at[2 + 2 * heads + heads // 2])
    inv_copy.start()
    kv_copies = []
    for h in range(heads):
        cols = pl.ds(h * HEAD, HEAD)
        pair = (
            pltpu.make_async_copy(wk_hbm.at[:, cols], wkv.at[h, :, pl.ds(0, HEAD)], load_sem.at[1 + 2 * h]),
            pltpu.make_async_copy(wv_hbm.at[:, cols], wkv.at[h, :, pl.ds(HEAD, HEAD)], load_sem.at[2 + 2 * h]),
        )
        for copy in pair:
            copy.start()
        kv_copies.append(pair)
    q_copies = []
    for p in range(heads // 2):
        copy = pltpu.make_async_copy(
            wq_hbm.at[:, pl.ds(p * 2 * HEAD, 2 * HEAD)], wq.at[p], load_sem.at[1 + 2 * heads + p])
        copy.start()
        q_copies.append(copy)
    wo_copy = pltpu.make_async_copy(wo_hbm, wo, load_sem.at[1 + 2 * heads + heads // 2])
    wo_copy.start()

    barrier = pltpu.get_barrier_semaphore()
    y_partner = sp + 1 - 2 * odd

    def greet(ids):
        pl.semaphore_signal(barrier, inc=1, device_id=ids, device_id_type=MESH)

    greet({"tp": other})
    greet({"sp": y_partner})

    @pl.when(has_next)
    def _():
        greet({"sp": sp + 2})

    @pl.when(z > 0)
    def _():
        greet({"sp": sp - 2})

    row = iota((256, 256), 0)
    perm[...] = jnp.where(spot(row & 63) + (row >> 6) == iota((256, 256), 1), 1.0, 0.0).astype(BF16)

    pl.semaphore_wait(barrier, 2 + has_next.astype(jnp.int32) + (z > 0).astype(jnp.int32))

    tok_copy.wait()
    width = tok.shape[1]

    def reorder(i, _):
        cols = pl.ds(pl.multiple_of(i * 512, 512), 512)
        moved = jnp.dot(perm[...], tok[:, cols], preferred_element_type=F32).astype(BF16)
        xg[:, tp, :, cols] = moved.reshape(CLASSES, 64, 512)
        return 0

    lax.fori_loop(0, width // 512, reorder, 0)
    x_copy = pltpu.make_async_remote_copy(
        src_ref=xg.at[:, tp], dst_ref=xg.at[:, tp], send_sem=x_sem.at[0], recv_sem=x_sem.at[1],
        device_id={"tp": other}, device_id_type=MESH)
    x_copy.start()

    inv_copy.wait()
    lane = iota((128, HEAD), 1)

    def table(c, _):
        positions = sp * 512 + spot(iota((128, HEAD), 0)) + c
        angles = positions.astype(F32) * inv[...]
        rows = pl.ds(pl.multiple_of(c * 128, 128), 128)
        cos_ref[rows, :] = jnp.cos(angles)
        sine = jnp.sin(angles)
        sin_ref[rows, :] = jnp.where(lane < HEAD // 2, -sine, sine)
        return 0

    lax.fori_loop(0, CLASSES, table, 0)

    def remote(src, dst, send_sem, recv_sem, ids):
        return pltpu.make_async_remote_copy(
            src_ref=src, dst_ref=dst, send_sem=send_sem, recv_sem=recv_sem,
            device_id=ids, device_id_type=MESH)

    down = {"sp": sp + 2}
    up = {"sp": sp - 2}
    side = {"sp": y_partner}

    def send(h, src, dst, ids):
        return remote(ctx.at[h, :, :, src], ctx.at[h, :, :, dst],
                      ctx_send.at[dst, h], ctx_recv.at[dst, h], ids)

    def send_own(h):
        return ((has_next, send(h, O, A, down)), (even, send(h, O, C, side)))

    def send_relay(h):
        return (((odd == 1) & (z > 0), send(h, A, C, side)),)

    def send_query(h):
        return ((z > 0, remote(q.at[h], visitor.at[h], q_sem.at[0, h], q_sem.at[1, h], up)),)

    def send_part(h):
        return ((has_next, remote(part.at[h], far_out.at[h], part_sem.at[0, h], part_sem.at[1, h], down)),
                (has_next, remote(part_lse.at[h], far_lse.at[h], lse_sem.at[0, h], lse_sem.at[1, h], down)))

    def start_all(sends):
        for condition, copy in sends:
            @pl.when(condition)
            def _():
                copy.start()

    def receive(h, slot):
        @pl.when(sp >= 2 - slot)
        def _():
            send(h, slot, slot, side).wait_recv()

    x_copy.wait_recv()

    def tokens():
        return xg[...].reshape(512, width)

    def project_kv(h, _):
        kv = jnp.dot(tokens(), wkv[h], preferred_element_type=F32)
        k = rotated(kv[:, :HEAD], cos_ref[...], sin_ref[...]).astype(BF16)
        ctx[h, 0, :, O] = k.reshape(CLASSES, 128, HEAD)
        ctx[h, 1, :, O] = kv[:, HEAD:].astype(BF16).reshape(CLASSES, 128, HEAD)
        start_all(send_own(h))
        return 0

    for pair in kv_copies:
        for copy in pair:
            copy.wait()
    lax.fori_loop(0, heads, project_kv, 0)

    for copy in q_copies:
        copy.wait()

    def project_q(p, _):
        qq = jnp.dot(tokens(), wq[p], preferred_element_type=F32)
        for s in range(2):
            r = rotated(qq[:, s * HEAD:(s + 1) * HEAD], cos_ref[...], sin_ref[...])
            q[2 * p + s] = r.astype(BF16).reshape(CLASSES, 128, HEAD)
            start_all(send_query(2 * p + s))
        return 0

    lax.fori_loop(0, heads // 2, project_q, 0)

    qi, kj = iota((128, 640), 0), iota((128, 640), 1)
    dist = 4 - (kj >> 7)
    diff = spot(qi) - spot(kj & 127) + 512 * dist
    here = (dist <= sp) | ((dist >= 3) & (dist <= sp + 2))
    far = here & ((diff & 15) == 0) & (diff >= 0) & (diff <= FAR_DILATION * REACH_STEPS)
    b16[...] = jnp.where(far, 0.0, NEG)
    mid = here & (diff >= 0) & (diff <= MIDDLE_DILATION * REACH_STEPS)
    b4[...] = jnp.where(mid, 0.0, NEG)[:, 384:]
    key_spot = jnp.where(kj < 128, kj - 128, spot(kj & 127) + ((kj >> 7) - 1))
    for c in range(CLASSES):
        near = spot(qi) + c - key_spot
        ok = (near >= 0) & (near <= REACH_STEPS) & ((kj >= 128) | (sp > 0))
        b1[c] = jnp.where(ok, 0.0, NEG)
    col = iota((512, 512), 1)
    unperm[...] = jnp.where(spot(col & 127) + (col >> 7) == iota((512, 512), 0), 1.0, 0.0).astype(BF16)

    for slot in (A, C):
        @pl.when(sp < 2 - slot)
        def _():
            def clear(h, _):
                ctx[h, :, :, slot] = jnp.zeros((2, CLASSES, 128, HEAD), BF16)
                return 0
            lax.fori_loop(0, heads, clear, 0)

    part_lse[...] = jnp.zeros(part_lse.shape, F32)

    @pl.when(z == 0)
    def _():
        far_out[...] = jnp.zeros(far_out.shape, BF16)
        far_lse[...] = jnp.full(far_lse.shape, NEG, F32)

    def mix_copy(h):
        cols = pl.ds(pl.multiple_of(h * HEAD, HEAD), HEAD)
        return pltpu.make_async_remote_copy(
            src_ref=mixg.at[tp, :, cols], dst_ref=mixg.at[tp, :, cols],
            send_sem=mix_send.at[h], recv_sem=mix_recv.at[h],
            device_id={"tp": other}, device_id_type=MESH)

    eye = iota((128, 128), 0) == iota((128, 128), 1)

    def visit(h):
        @pl.when(has_next)
        def _():
            remote(q.at[h], visitor.at[h], q_sem.at[0, h], q_sem.at[1, h], side).wait_recv()

            def of_class(c, _):
                keys = ctx[h, 0, c, A:O].reshape(2 * 128, HEAD)
                vals = ctx[h, 1, c, A:O].reshape(2 * 128, HEAD)
                scores = transposed_dot(visitor[h, c], keys) * HEAD ** (-0.5)
                result, lse = softmax(scores + b16[:, :256], vals)
                part[h, c] = result.astype(BF16)
                part_lse[h, pl.ds(c, 1), :] = jnp.sum(jnp.where(eye, lse, 0.0), axis=0, keepdims=True)
                return 0

            lax.fori_loop(0, CLASSES, of_class, 0)

        start_all(send_part(h))

    def attend(h):
        tail = unperm[384:512, :]
        for kv, near in ((0, k1), (1, v1)):
            last = ctx[h, kv, :, C].reshape(512, HEAD)
            near[0:128] = jnp.dot(tail, last, preferred_element_type=F32).astype(BF16)
            near[128:640] = ctx[h, kv, :, O].reshape(512, HEAD)

        def of_class(c, _):
            qc = q[h, c]
            keys = ctx[h, 0, c].reshape(SLOTS * 128, HEAD)
            vals = ctx[h, 1, c].reshape(SLOTS * 128, HEAD)
            scores = transposed_dot(qc, keys) * HEAD ** (-0.5)
            r16, l16 = softmax(scores + b16[:, 256:], vals)
            r4, l4 = softmax(scores[:, 128:] + b4[...], vals[128:])
            r1, l1 = softmax(transposed_dot(qc, k1[...]) * HEAD ** (-0.5) + b1[c], v1[...])
            most = jnp.maximum(jnp.maximum(l16, l4), l1)
            e16, e4, e1 = jnp.exp(l16 - most), jnp.exp(l4 - most), jnp.exp(l1 - most)
            total = e16 + e4 + e1
            share = 1.0 / total
            near_out[h, c] = r1 * (e1 * share) + r4 * (e4 * share) + r16 * (e16 * share)
            near_lse[h, c] = jnp.broadcast_to(most + jnp.log(total), (128, HEAD))
            return 0

        lax.fori_loop(0, CLASSES, of_class, 0)

    def step(h, _):
        @pl.when(h < heads)
        def _():
            receive(h, A)
            start_all(send_relay(h))

        @pl.when(h > 0)
        def _():
            receive(h - 1, C)
            visit(h - 1)

        @pl.when((h > 0) & (h < heads))
        def _():
            attend(h - 1)
        return 0

    lax.fori_loop(0, heads + 1, step, 0)

    def combine(h):
        @pl.when(z > 0)
        def _():
            remote(part.at[h], far_out.at[h], part_sem.at[0, h], part_sem.at[1, h], side).wait_recv()
            remote(part_lse.at[h], far_lse.at[h], lse_sem.at[0, h], lse_sem.at[1, h], side).wait_recv()

        for c in range(CLASSES):
            row = far_lse[h, c:c + 1, :]
            lf = jnp.sum(jnp.where(eye, row, 0.0), axis=1, keepdims=True)
            ln = near_lse[h, c]
            most = jnp.maximum(ln, lf)
            en, ef = jnp.exp(ln - most), jnp.exp(lf - most)
            mixed = (near_out[h, c] * en + far_out[h, c].astype(F32) * ef) / (en + ef)
            mixp[c * 128:(c + 1) * 128, :] = mixed.astype(BF16)
        natural = jnp.dot(unperm[...], mixp[...], preferred_element_type=F32).astype(BF16)
        cols = pl.ds(pl.multiple_of(h * HEAD, HEAD), HEAD)
        mixg[tp, :, cols] = natural
        mix_copy(h).start()

    def gathered(h, _):
        mix_copy(h).wait_recv()
        return 0

    half = mixg.shape[2]
    first = half // 2

    def partial_out(i, _):
        cols = pl.ds(pl.multiple_of(i * 256, 256), 256)
        total = jnp.dot(mixg[0, :, :first], wo[:first, cols], preferred_element_type=F32)
        total = total + jnp.dot(mixg[1, :, :first], wo[half:half + first, cols], preferred_element_type=F32)
        out_sum[:, cols] = total
        return 0

    def finish(h, _):
        @pl.when(h == heads - 2)
        def _():
            attend(heads - 1)

        @pl.when(h == heads - 1)
        def _():
            wo_copy.wait()
            lax.fori_loop(0, heads // 2, gathered, 0)
            lax.fori_loop(0, out_ref.shape[1] // 256, partial_out, 0)

        combine(h)
        return 0

    lax.fori_loop(0, heads, finish, 0)

    lax.fori_loop(heads // 2, heads, gathered, 0)

    def project_out(i, _):
        cols = pl.ds(pl.multiple_of(i * 256, 256), 256)
        total = jnp.dot(mixg[0, :, first:], wo[first:half, cols], preferred_element_type=F32)
        total = total + jnp.dot(mixg[1, :, first:], wo[half + first:, cols], preferred_element_type=F32)
        out_ref[:, cols] = (out_sum[:, cols] + total).astype(BF16)
        return 0

    lax.fori_loop(0, out_ref.shape[1] // 256, project_out, 0)

    x_copy.wait_send()

    def left(h, _):
        for sends in (send_own(h), send_relay(h), send_query(h), send_part(h)):
            for condition, copy in sends:
                @pl.when(condition)
                def _():
                    copy.wait_send()
        mix_copy(h).wait_send()
        return 0

    lax.fori_loop(0, heads, left, 0)


def body(tokens, query_weight, key_weight, value_weight, output_weight):
    n_sp = lax.axis_size("sp")
    half_rows, width = tokens.shape
    rows = half_rows * lax.axis_size("tp")
    heads = query_weight.shape[1] // HEAD
    assert rows * 4 == FAR_DILATION * REACH_STEPS and rows == 512
    assert n_sp % 2 == 0 and lax.axis_size("tp") == 2 and heads % 2 == 0 and heads >= 4

    half = HEAD // 2
    inverse = THETA_BASE ** (-np.arange(half, dtype=np.float64) / half)
    inverse = np.concatenate([inverse, inverse]).astype(np.float32)[None, :]

    anywhere = pl.BlockSpec(memory_space=pl.ANY)
    vmem = pl.BlockSpec(memory_space=pltpu.VMEM)
    out_cols = output_weight.shape[1]
    return pl.pallas_call(
        functools.partial(kernel, n_sp, heads),
        out_shape=jax.ShapeDtypeStruct((rows, out_cols), BF16),
        in_specs=[anywhere] * 6,
        out_specs=vmem,
        scratch_shapes=[
            pltpu.VMEM((half_rows, width), BF16),
            pltpu.VMEM((heads, width, 2 * HEAD), BF16),
            pltpu.VMEM((heads // 2, width, 2 * HEAD), BF16),
            pltpu.VMEM(output_weight.shape, BF16),
            pltpu.VMEM((1, HEAD), F32),
            pltpu.VMEM((rows, HEAD), F32),
            pltpu.VMEM((rows, HEAD), F32),
            pltpu.VMEM((CLASSES, 2, 64, width), BF16),
            pltpu.VMEM((heads, 2, CLASSES, SLOTS, 128, HEAD), BF16),
            pltpu.VMEM((heads, CLASSES, 128, HEAD), BF16),
            pltpu.VMEM((heads, CLASSES, 128, HEAD), BF16),
            pltpu.VMEM((640, HEAD), BF16),
            pltpu.VMEM((640, HEAD), BF16),
            pltpu.VMEM((256, 256), BF16),
            pltpu.VMEM((512, 512), BF16),
            pltpu.VMEM((128, 640), F32),
            pltpu.VMEM((128, 256), F32),
            pltpu.VMEM((CLASSES, 128, 640), F32),
            pltpu.VMEM((heads, CLASSES, 128, HEAD), F32),
            pltpu.VMEM((heads, CLASSES, 128, HEAD), F32),
            pltpu.VMEM((heads, CLASSES, 128, HEAD), BF16),
            pltpu.VMEM((heads, 8, 128), F32),
            pltpu.VMEM((heads, CLASSES, 128, HEAD), BF16),
            pltpu.VMEM((heads, 8, 128), F32),
            pltpu.VMEM((512, HEAD), BF16),
            pltpu.VMEM((2, rows, heads * HEAD), BF16),
            pltpu.VMEM((rows, out_cols), F32),
            pltpu.SemaphoreType.DMA((3 + 2 * heads + heads // 2,)),
            pltpu.SemaphoreType.DMA((2,)),
            pltpu.SemaphoreType.DMA((2, heads)),
            pltpu.SemaphoreType.DMA((2, heads)),
            pltpu.SemaphoreType.DMA((2, heads)),
            pltpu.SemaphoreType.DMA((2, heads)),
            pltpu.SemaphoreType.DMA((2, heads)),
            pltpu.SemaphoreType.DMA((heads,)),
            pltpu.SemaphoreType.DMA((heads,)),
        ],
        compiler_params=pltpu.CompilerParams(
            collective_id=0, has_side_effects=True, vmem_limit_bytes=63 * 1024 * 1024
        ),
    )(tokens, query_weight, key_weight, value_weight, output_weight, jnp.asarray(inverse))


def solution(mesh):
    in_specs = (
        P(("grp", "sp", "tp"), None),
        P(None, "tp"),
        P(None, "tp"),
        P(None, "tp"),
        P(None, "tp"),
    )
    out_specs = P(("grp", "sp"), "tp")
    return jax.shard_map(body, mesh=mesh, in_specs=in_specs, out_specs=out_specs, check_vma=False)
```
